32 devices in a mesh: sp: 8 (over z, y), tp: 4 (over x, core).
Axes of the slice: x: 2, y: 2, z: 4, core: 2. Of those that a mesh axis runs over, the one named last changes fastest.
Arguments:
- activations: bfloat16 [3584, 2048], P(('sp', 'tp')), may hold values from -27.5 to 27.5
- query_weight: bfloat16 [2048, 2048], P(None, 'tp'), may hold values from -0.088388348 to 0.088388348
- key_weight: bfloat16 [2048, 2048], P(None, 'tp'), may hold values from -0.088388348 to 0.088388348
- value_weight: bfloat16 [2048, 2048], P(None, 'tp'), may hold values from -0.125 to 0.125
- out_weight: bfloat16 [2048, 2048], P('tp'), may hold values from -0.125 to 0.125
- lambdas: float32 [8], P('tp'), may hold values from 0.3 to 0.8
- head_gain: float32 [256], replicated, may hold values from 0.1 to 1.9
Outputs:
- mixed: bfloat16 [3584, 2048], P(('sp', 'tp'))
The draws below stay inside these ranges and needn't reach their ends.
All inputs are finite; a program needn't handle non-finite values.
Results may differ from the reference program's by a relative error of at most 0.014.
Values may be sent and summed in bfloat16 or wider, within the bound.
A program may use at most 128 MiB of HBM per device.

```python
import jax
import jax.numpy as jnp
from jax import lax

D = 2048
HEADS = 8
HEAD = 128
VALUE = 256
TOK_DEV = 448
SEQ = 3584
N_TP = 4


def draw_activations(key, part):
    noise_base = jnp.clip(jax.random.normal(jax.random.fold_in(key, 1), (SEQ, D), jnp.float32), -4.0, 4.0)
    block_means = jax.random.uniform(jax.random.fold_in(key, 2), (SEQ // TOK_DEV, D), jnp.float32, -1.5, 1.5)
    result = noise_base + jnp.repeat(block_means, TOK_DEV, axis=0)
    return result.astype(jnp.bfloat16)


def paired_weights(key):
    bound_value = 4.0 * D ** (-0.5)
    first_draw = jax.random.normal(jax.random.fold_in(key, 11), (D, HEADS * 2 * HEAD), jnp.float32) * D ** (-0.5)
    second = jax.random.normal(jax.random.fold_in(key, 12), (D, HEADS * 2 * HEAD), jnp.float32) * D ** (-0.5)
    return (first_draw, second, bound_value)


def draw_query_weight(key, part):
    first_draw, second, bound_value = paired_weights(key)
    return jnp.clip(first_draw, -bound_value, bound_value).astype(jnp.bfloat16)


def draw_key_weight(key, part):
    first_draw, second, bound_value = paired_weights(key)
    mixed_draw = second
    return jnp.clip(mixed_draw, -bound_value, bound_value).astype(jnp.bfloat16)


def level_of(key, shape, shards, least, largest):
    gain = 1.0
    for dim, blocks in shards:
        draws = jax.random.uniform(jax.random.fold_in(jax.random.fold_in(key, 6), dim), (blocks,), jnp.float32, least / len(shards), largest / len(shards))
        gain = gain * jnp.repeat(jnp.exp(draws), shape[dim] // blocks).reshape((-1,) + (1,) * (len(shape) - 1 - dim))
    return gain


def bell_draw(stream_key, dims, deviation, reach, split=(), kind=jnp.bfloat16):
    values = jax.random.normal(stream_key, dims, jnp.float32) * deviation
    if len(split) > 0:
        values = level_of(stream_key, dims, split, -0.22, 0.18) * values
    return jnp.clip(values, min=-reach, max=reach).astype(kind)


def setup_inputs(seed: int = 0) -> dict:
    key_of = jax.random.split(jax.random.key(seed), 8)
    activations = draw_activations(jax.random.fold_in(key_of[7], 71), 0)
    query_weight = draw_query_weight(jax.random.fold_in(key_of[7], 71), 0)
    key_weight = draw_key_weight(jax.random.fold_in(key_of[7], 71), 0)
    value_weight = bell_draw(key_of[3], (D, HEADS * VALUE), D ** -0.5, 0.125, ((1, 4),))
    out_weight = bell_draw(key_of[4], (HEADS * VALUE, D), (HEADS * VALUE) ** -0.5, 0.125, ((0, 4),))
    lambdas = jnp.clip(0.3 + 0.5 * jax.random.uniform(key_of[5], (HEADS,), jnp.float32) ** level_of(key_of[5], (HEADS,), ((0, 4),), -0.2, 0.2), 0.3, 0.8)
    head_gain = jnp.clip(1.0 + 0.18 * jax.random.normal(key_of[6], (VALUE,), jnp.float32), 0.1, 1.9)
    return dict(activations=activations, query_weight=query_weight, key_weight=key_weight, value_weight=value_weight, out_weight=out_weight, lambdas=lambdas, head_gain=head_gain)


norm_floor = 0.02

def reference(activations, query_weight, key_weight, value_weight, out_weight, lambdas, head_gain):
    queries = jnp.dot(activations, query_weight, preferred_element_type=jnp.float32).astype(jnp.bfloat16)
    key_rows = jnp.dot(activations, key_weight, preferred_element_type=jnp.float32).astype(jnp.bfloat16)
    value_rows = jnp.dot(activations, value_weight, preferred_element_type=jnp.float32).astype(jnp.bfloat16)
    queries = queries.reshape(SEQ, HEADS, 2, HEAD).transpose(1, 0, 2, 3)
    key_rows = key_rows.reshape(SEQ, HEADS, 2, HEAD).transpose(1, 0, 2, 3)
    value_rows = value_rows.reshape(SEQ, HEADS, VALUE).transpose(1, 0, 2)
    blocks = SEQ // TOK_DEV
    score_scale = HEAD ** (-0.5)
    key_pos = jnp.arange(SEQ, dtype=jnp.int32)

    def one_block(index):
        head_index = index // blocks
        block_index = index % blocks
        first_row = (block_index * TOK_DEV).astype(jnp.int32)
        query_rows = lax.dynamic_slice_in_dim(queries[head_index], first_row, TOK_DEV, 0).astype(jnp.float32)
        key_all = key_rows[head_index].astype(jnp.float32)
        value_all = value_rows[head_index].astype(jnp.float32)
        scores = jnp.einsum('qme,kme->mqk', query_rows, key_all) * score_scale
        query_pos = first_row + jnp.arange(TOK_DEV, dtype=jnp.int32)
        allowed = key_pos[None, :] <= query_pos[:, None]
        masked = jnp.where(allowed[None], scores, -jnp.inf)
        row_top = lax.optimization_barrier(jnp.max(masked, axis=-1, keepdims=True))
        exp_weights = jnp.where(allowed[None], jnp.exp(masked - row_top), 0.0)
        denominators = lax.optimization_barrier(jnp.sum(exp_weights, axis=-1))
        rounded = lax.optimization_barrier(exp_weights.astype(jnp.bfloat16)).astype(jnp.float32)
        weighted = jnp.einsum('mqk,kv->mqv', rounded, value_all)
        lambda_head = lambdas[head_index]
        combined = weighted[0] / denominators[0][:, None] - lambda_head * weighted[1] / denominators[1][:, None]
        inverse_rms = lax.rsqrt(lax.optimization_barrier(jnp.mean(combined * combined, axis=-1, keepdims=True)) + norm_floor)
        return (combined * inverse_rms * head_gain).astype(jnp.bfloat16)
    heads_out = lax.map(one_block, jnp.arange(HEADS * blocks, dtype=jnp.int32))
    heads_out = heads_out.reshape(HEADS, SEQ, VALUE).transpose(1, 0, 2).reshape(SEQ, HEADS * VALUE)
    group_width = HEADS // N_TP * VALUE
    totals = jnp.zeros((SEQ, D), jnp.float32)
    for group_index in range(N_TP):
        columns = heads_out[:, group_index * group_width:(group_index + 1) * group_width]
        weight_rows = out_weight[group_index * group_width:(group_index + 1) * group_width]
        partial_value = jnp.dot(columns, weight_rows, preferred_element_type=jnp.float32).astype(jnp.bfloat16)
        totals = totals + partial_value.astype(jnp.float32)
    return totals.astype(jnp.bfloat16)
```

```python
import functools
import math

import jax
import jax.numpy as jnp
from jax import lax
from jax.experimental import pallas as pl
from jax.experimental.pallas import tpu as pltpu
from jax.sharding import PartitionSpec as P

HEAD = 128
VALUE = 256


norm_floor = 0.02
very_low = -1e30
MESH = pl.DeviceIdType.MESH


def layer_kernel(
    S, T, L, R,
    act, qw, kw, vw, ow, lam_in, gain,
    out,
    A, WP, W, PR, PC, KV, HO, HI, LB, ACC, MX, DN, TOT,
    w_sem, own_sem, a_send, a_recv, lam_send, lam_recv, o_send, o_recv,
    p_send, p_recv, f_send, f_recv, h_send, h_recv,
):
    X = T // 2
    half = T // 2
    s = lax.axis_index("sp")
    t = lax.axis_index("tp")
    x = t // 2
    c = t % 2
    mate = x * 2 + (1 - c)
    hl = s // half
    r = (s % half) * 2 + c
    head = x * 2 * L + hl
    width = L * 256

    def remote(src, dst, ss, rs, sp, tp):
        return pltpu.make_async_remote_copy(
            src_ref=src, dst_ref=dst, send_sem=ss, recv_sem=rs,
            device_id=(sp, tp), device_id_type=MESH,
        )

    def weight_copies():
        return [
            pltpu.make_async_copy(ref, WP.at[k], w_sem.at[k])
            for k, ref in enumerate((qw, kw, vw))
        ]

    def own_copies():
        return [
            pltpu.make_async_copy(act, A.at[t], own_sem.at[0]),
            pltpu.make_async_copy(ow, W.at[pl.ds(t * L, L)], own_sem.at[1]),
            pltpu.make_async_copy(lam_in, LB.at[c], own_sem.at[2]),
        ]

    def act_out(k):
        if k == 0:
            return remote(act, A.at[t], a_send.at[0], a_recv.at[t], s, mate)
        return remote(act, A.at[t], a_send.at[k], a_recv.at[t], s, ((x + k) % X) * 2 + c)

    def act_pass(k):
        src = ((x + k) % X) * 2 + c
        return remote(A.at[src], A.at[src], a_send.at[X - 1 + k], a_recv.at[src], s, mate)

    def ow_part(i):
        return pl.ds(i * L, L)

    def ow_out(k):
        dst = mate if k == 0 else ((x + k) % X) * 2 + c
        return remote(ow, W.at[ow_part(t)], o_send.at[k], o_recv.at[t], s, dst)

    def ow_pass(k):
        src = ((x + k) % X) * 2 + c
        return remote(
            W.at[ow_part(src)], W.at[ow_part(src)],
            o_send.at[X - 1 + k], o_recv.at[src], s, mate,
        )

    lam_out = remote(lam_in, LB.at[c], lam_send.at[0], lam_recv.at[0], s, mate)

    for k in range(1, X):
        act_out(k).start()
    act_out(0).start()
    for copy in weight_copies():
        copy.start()
    for copy in own_copies():
        copy.start()
    lam_out.start()
    for k in range(1, X):
        ow_out(k).start()
    ow_out(0).start()

    def piece_place(l, q):
        return (c * L + l) * half + q // 2, x * 2 + q % 2

    def piece(l, q):
        sp, tp = piece_place(l, q)
        return remote(
            PR.at[l, q], PC.at[s], p_send.at[l, q], p_recv.at[s], sp, tp
        )

    def piece_here(l, q):
        return pltpu.make_async_copy(PR.at[l, q], PC.at[s], p_recv.at[s])

    def send_piece(l, q):
        sp, tp = piece_place(l, q)
        here = (sp == s) & (tp == t)

        @pl.when(here)
        def _():
            piece_here(l, q).start()

        @pl.when(jnp.logical_not(here))
        def _():
            piece(l, q).start()

    def project(k, carry):
        xx = (x + k) % X
        rows = A[pl.ds(xx * 2, 2)].reshape(2 * R, A.shape[2])
        for part in range(3):
            got = jnp.dot(rows, WP[part], preferred_element_type=jnp.float32)
            got = got.astype(jnp.bfloat16)
            for l in range(L):
                cols = got[:, l * 256:(l + 1) * 256]
                PR[l, pl.ds(xx * 2, 2), :, part * 256:(part + 1) * 256] = cols.reshape(2, R, 256)
        for l in range(L):
            for q in range(2):
                send_piece(l, xx * 2 + q)
        return carry

    def wait_act(i):
        remote(act, A.at[i], a_send.at[0], a_recv.at[i], s, mate).wait_recv()

    own_copies()[0].wait()
    for copy in weight_copies():
        copy.wait()
    wait_act(mate)
    project(0, 0)
    for k in range(1, X):
        wait_act(((x + k) % X) * 2 + c)
        act_pass(k).start()
        wait_act(((x + k) % X) * 2 + (1 - c))
        project(k, 0)

    span = T * R

    def kv_row(block, member):
        return pl.ds(block * span + member * R, R)

    def kv_copy(kind, block, member, src, sp, tp):
        return remote(
            src, KV.at[kv_row(block, member)],
            f_send.at[kind, block], f_recv.at[block, member], sp, tp,
        )

    def on_chip_row(y):
        return hl * half + y

    y = s % half

    def spread_own(block):
        return [
            kv_copy(0, block, r, PC.at[block, :, 256:768], s, mate)
        ] + [
            kv_copy(k, block, r, PC.at[block, :, 256:768], on_chip_row((y + k) % half), t)
            for k in range(1, half)
        ]

    def pass_on(block, k):
        member = ((y + k) % half) * 2 + c
        return kv_copy(
            half - 1 + k, block, member, KV.at[kv_row(block, member)], s, mate
        )

    def kv_here(block):
        return pltpu.make_async_copy(
            PC.at[block, :, 256:768], KV.at[kv_row(block, r)], f_recv.at[block, r]
        )

    def wait_kv(block, member):
        kv_copy(0, block, member, PC.at[block, :, 256:768], s, mate).wait_recv()

    def wait_piece(block):
        remote(PR.at[0, 0], PC.at[block], p_send.at[0, 0], p_recv.at[block], s, mate).wait_recv()

    def order(i):
        return (hl * half + i) % S

    def forward(i, carry):
        block = order(i)
        wait_piece(block)
        for copy in spread_own(block)[::-1]:
            copy.start()
        kv_here(block).start()
        return carry

    def relay(i, carry):
        block = order(i)
        for k in range(1, half):
            wait_kv(block, ((y + k) % half) * 2 + c)
            pass_on(block, k).start()
        return carry

    def both(i, carry):
        forward(i, carry)

        @pl.when(i > 0)
        def _():
            relay(i - 1, carry)

        return carry

    lax.fori_loop(0, S, both, 0)
    relay(S - 1, 0)

    own_copies()[2].wait()
    lam_out.wait_recv()
    pair = 2
    q_rows = pair * R
    k_rows = pair * span
    scale = HEAD ** (-0.5) * math.log2(math.e)

    def wait_block(block):
        kv_here(block).wait()
        for k in range(half):
            if k > 0:
                pass
            wait_kv(block, ((y + k) % half) * 2 + (1 - c))

    def home(block):
        return remote(
            HO.at[block], HI.at[head], h_send.at[block], h_recv.at[head], block, r
        )

    def home_here(block):
        return pltpu.make_async_copy(HO.at[block], HI.at[head], h_recv.at[head])

    def chunk(i, j, masked):
        for m in range(2):
            q = PC[pl.ds(i * pair, pair), :, m * 128:(m + 1) * 128].reshape(q_rows, 128)
            keys = KV[pl.ds(j * k_rows, k_rows), m * 128:(m + 1) * 128]
            sc = lax.dot_general(
                q, keys, (((1,), (1,)), ((), ())), preferred_element_type=jnp.float32
            ) * scale
            if masked:
                row = lax.broadcasted_iota(jnp.int32, (q_rows, k_rows), 0)
                col = lax.broadcasted_iota(jnp.int32, (q_rows, k_rows), 1)
                pos = row + r * R
                for b in range(1, pair):
                    pos = pos + jnp.where(row >= b * R, span - R, 0)
                sc = jnp.where(col <= pos, sc, very_low)
            old = MX[m, :, :1]
            new = jnp.maximum(old, jnp.max(sc, axis=1, keepdims=True))
            p = jnp.exp2(sc - new)
            factor = jnp.exp2(old - new)
            total = DN[m, :, :1] * factor + jnp.sum(p, axis=1, keepdims=True)
            values = KV[pl.ds(j * k_rows, k_rows), 256:512]
            got = jnp.dot(p.astype(jnp.bfloat16), values, preferred_element_type=jnp.float32)
            ACC[m] = ACC[m] * factor + got
            MX[m] = jnp.broadcast_to(new, MX.shape[1:])
            DN[m] = jnp.broadcast_to(total, DN.shape[1:])

    lam = LB[hl // L, hl % L][:1, :1]

    def tile(i, carry):
        for b in range(pair):
            wait_block(i * pair + b)
        MX[...] = jnp.full(MX.shape, very_low, jnp.float32)
        DN[...] = jnp.zeros(DN.shape, jnp.float32)
        ACC[...] = jnp.zeros(ACC.shape, jnp.float32)

        def inner(j, carry2):
            chunk(i, j, False)
            return carry2

        lax.fori_loop(0, i, inner, 0)
        chunk(i, i, True)
        comb = ACC[0] / DN[0, :, :1] - lam * (ACC[1] / DN[1, :, :1])
        inv = lax.rsqrt(jnp.mean(comb * comb, axis=1, keepdims=True) + norm_floor)
        normed = (comb * inv * gain[...]).astype(jnp.bfloat16)
        HO[pl.ds(i * pair, pair)] = normed.reshape(pair, R, 256)
        for b in range(pair):
            block = i * pair + b
            here = (block == s) & (r == t)

            @pl.when(here)
            def _():
                home_here(block).start()

            @pl.when(jnp.logical_not(here))
            def _():
                home(block).start()

        return carry

    lax.fori_loop(0, S // pair, tile, 0)

    def wait_ow(i):
        remote(ow, W.at[ow_part(i)], o_send.at[0], o_recv.at[i], s, mate).wait_recv()

    own_copies()[1].wait()
    for k in range(1, X):
        wait_ow(((x + k) % X) * 2 + c)
        ow_pass(k).start()
    wait_ow(mate)
    for k in range(1, X):
        wait_ow(((x + k) % X) * 2 + (1 - c))

    TOT[...] = jnp.zeros(TOT.shape, jnp.float32)

    def add_head(i, carry):
        remote(HO.at[0], HI.at[i], h_send.at[0], h_recv.at[i], s, mate).wait_recv()
        TOT[...] += jnp.dot(HI[i], W[i], preferred_element_type=jnp.float32)
        return carry

    lax.fori_loop(0, T * L, add_head, 0)
    out[...] = TOT[...].astype(jnp.bfloat16)

    lam_out.wait_send()
    for k in range(X):
        act_out(k).wait_send()
        ow_out(k).wait_send()
    for k in range(1, X):
        act_pass(k).wait_send()
        ow_pass(k).wait_send()
    for l in range(L):
        for q in range(T):
            sp, tp = piece_place(l, q)

            @pl.when(jnp.logical_not((sp == s) & (tp == t)))
            def _():
                piece(l, q).wait_send()

    def drain(block, carry):
        for copy in spread_own(block):
            copy.wait_send()
        for k in range(1, half):
            pass_on(block, k).wait_send()

        @pl.when(jnp.logical_not((block == s) & (r == t)))
        def _():
            home(block).wait_send()

        return carry

    lax.fori_loop(0, S, drain, 0)


def fused(S, T, L, activations, query_weight, key_weight, value_weight, out_weight, lambdas, head_gain):
    R, D = activations.shape
    X = T // 2
    half = T // 2
    bf, f32 = jnp.bfloat16, jnp.float32
    vmem = pl.BlockSpec(memory_space=pltpu.VMEM)
    hbm = pl.BlockSpec(memory_space=pl.ANY)
    dma = pltpu.SemaphoreType.DMA
    lam_in = jnp.broadcast_to(lambdas[:, None, None], (L, 8, 128))
    width = query_weight.shape[1]
    return pl.pallas_call(
        functools.partial(layer_kernel, S, T, L, R),
        out_shape=jax.ShapeDtypeStruct((R, D), bf),
        in_specs=[vmem, hbm, hbm, hbm, hbm, vmem, vmem],
        out_specs=vmem,
        scratch_shapes=[
            pltpu.VMEM((T, R, D), bf),
            pltpu.VMEM((3, D, width), bf),
            pltpu.VMEM((T * L, VALUE, D), bf),
            pltpu.VMEM((L, T, R, 768), bf),
            pltpu.VMEM((S, R, 768), bf),
            pltpu.VMEM((S * T * R, 512), bf),
            pltpu.VMEM((S, R, VALUE), bf),
            pltpu.VMEM((T * L, R, VALUE), bf),
            pltpu.VMEM((2, L, 8, 128), f32),
            pltpu.VMEM((2, 2 * R, VALUE), f32),
            pltpu.VMEM((2, 2 * R, 128), f32),
            pltpu.VMEM((2, 2 * R, 128), f32),
            pltpu.VMEM((R, D), f32),
            dma((3,)), dma((3,)),
            dma((2 * X - 1,)), dma((T,)),
            dma((1,)), dma((1,)),
            dma((2 * X - 1,)), dma((T,)),
            dma((L, T)), dma((S,)),
            dma((2 * half - 1, S)), dma((S, T)),
            dma((S,)), dma((T * L,)),
        ],
        compiler_params=pltpu.CompilerParams(
            has_side_effects=True, vmem_limit_bytes=60 * 1024 * 1024
        ),
    )(
        activations, query_weight, key_weight, value_weight,
        out_weight.reshape(L, VALUE, D), lam_in, head_gain.reshape(1, VALUE),
    )


def empty_state(count, local_heads):
    return (
        jnp.full((local_heads, 2, count), very_low, jnp.float32),
        jnp.zeros((local_heads, 2, count), jnp.float32),
        jnp.zeros((local_heads, 2, count, VALUE), jnp.float32),
    )


def absorb(state, query_set, query_pos, key_block, value_block, key_first):
    running, denoms, accums = state
    local_heads = running.shape[0]
    span = key_block.shape[0]
    key_grid = key_block.reshape(span, local_heads, 2, HEAD)
    scores = jnp.einsum(
        "qhme,khme->hmqk", query_set, key_grid, preferred_element_type=jnp.float32
    ) * HEAD ** (-0.5)
    key_pos = key_first + jnp.arange(span, dtype=jnp.int32)
    allowed = key_pos[None, :] <= query_pos[:, None]
    masked = jnp.where(allowed, scores, very_low)
    updated = jnp.maximum(running, jnp.max(masked, axis=-1))
    exp_weights = jnp.where(allowed, jnp.exp(masked - updated[..., None]), 0.0)
    factor = jnp.exp(running - updated)
    denoms = denoms * factor + jnp.sum(exp_weights, axis=-1)
    value_grid = value_block.reshape(span, local_heads, VALUE)
    product = jnp.einsum(
        "hmqk,khv->hmqv",
        exp_weights.astype(jnp.bfloat16),
        value_grid,
        preferred_element_type=jnp.float32,
    )
    accums = accums * factor[..., None] + product
    return (updated, denoms, accums)


def make_folder(query_sets, carry, pieces):
    key_piece, value_piece = pieces
    length = key_piece.shape[0]
    span = math.gcd(length, 512)

    def one_span(span_index, states):
        offset = span_index * span
        key_block = lax.dynamic_slice_in_dim(key_piece, offset, span, 0)
        value_block = lax.dynamic_slice_in_dim(value_piece, offset, span, 0)
        fresh = []
        for state, query_entry in zip(states, query_sets):
            query_set, query_pos = query_entry

            def take(current):
                return absorb(current, query_set, query_pos, key_block, value_block, offset)

            def leave(current):
                return current

            fresh.append(lax.cond(offset <= query_pos[-1], take, leave, state))
        return tuple(fresh)

    return lax.fori_loop(0, length // span, one_span, carry)


def shards(activations, query_weight, key_weight, value_weight, out_weight, lambdas, head_gain):
    local_heads = lambdas.shape[0]
    query_width = query_weight.shape[1]
    joined_weight = jnp.concatenate([query_weight, key_weight, value_weight], axis=1)
    projected = jnp.dot(
        lax.all_gather(activations, "tp", axis=0, tiled=True),
        joined_weight,
        preferred_element_type=jnp.float32,
    ).astype(jnp.bfloat16)
    row_count = projected.shape[0]
    queries = projected[:, :query_width].reshape(row_count, local_heads, 2, HEAD)
    key_rows = projected[:, query_width : 2 * query_width]
    value_rows = projected[:, 2 * query_width :]
    position = lax.axis_index("sp") * row_count + jnp.arange(row_count, dtype=jnp.int32)
    query_sets = [(queries, position)]
    start_states = tuple((empty_state(entry[0].shape[0], local_heads) for entry in query_sets))
    finals = make_folder(
        query_sets,
        start_states,
        (
            lax.all_gather(key_rows, "sp", axis=0, tiled=True),
            lax.all_gather(value_rows, "sp", axis=0, tiled=True),
        ),
    )
    outputs = []
    for state in finals:
        running, denoms, accums = state
        combined = (
            accums[:, 0] / denoms[:, 0, :, None]
            - lambdas[:, None, None] * accums[:, 1] / denoms[:, 1, :, None]
        )
        inverse_rms = lax.rsqrt(jnp.mean(combined * combined, axis=-1, keepdims=True) + norm_floor)
        normed = (combined * inverse_rms * head_gain).astype(jnp.bfloat16)
        outputs.append(
            jnp.transpose(normed, (1, 0, 2)).reshape(normed.shape[1], local_heads * VALUE)
        )
    heads_out = outputs[0]
    return lax.psum_scatter(
        jnp.dot(heads_out, out_weight, preferred_element_type=jnp.float32).astype(jnp.bfloat16),
        "tp",
        scatter_dimension=0,
        tiled=True,
    )


def solution(mesh):
    in_specs = (
        P(("sp", "tp"), None),
        P(None, "tp"),
        P(None, "tp"),
        P(None, "tp"),
        P("tp", None),
        P("tp"),
        P(),
    )
    out_specs = P(("sp", "tp"), None)
    S, T = mesh.shape["sp"], mesh.shape["tp"]

    def layer(*args):
        L = args[5].shape[0] // T
        rows = args[0].shape[0] // (S * T)
        fits = T % 2 == 0 and S == L * T and S % 2 == 0 and rows % 16 == 0
        local = functools.partial(fused, S, T, L) if fits else shards
        return jax.shard_map(
            local, mesh=mesh, in_specs=in_specs, out_specs=out_specs, check_vma=False
        )(*args)

    return layer
```

```python
import functools
import math

import jax
import jax.numpy as jnp
from jax import lax
from jax.experimental import pallas as pl
from jax.experimental.pallas import tpu as pltpu
from jax.sharding import PartitionSpec as P

HEAD = 128
VALUE = 256


norm_floor = 0.02
very_low = -1e30
MESH = pl.DeviceIdType.MESH


def layer_kernel(
    S, T, L, R,
    act, qw, kw, vw, ow, lam_in, gain,
    out,
    A, WP, W, PR, PC, KV, HO, HI, LS, LB, ACC, MX, DN, TOT,
    w_sem, own_sem, a_send, a_recv, lam_send, lam_recv, o_send, o_recv, m_send, m_recv,
    p_send, p_recv, f_send, f_recv, h_send, h_recv,
):
    X, Y = 2, 2
    Z = S // Y
    s = lax.axis_index("sp")
    t = lax.axis_index("tp")
    x = t // 2
    c = t % 2
    y = s % Y
    z = s // Y
    mate = x * 2 + (1 - c)
    across = (1 - x) * 2 + c
    beside = z * Y + (1 - y)
    upper = z // (Z // 2)
    near = upper * (Z // 2)
    head = x * 2 * L + z
    span = T * R
    scale = HEAD ** (-0.5) * math.log2(math.e)

    def remote(src, dst, ss, rs, sp, tp):
        return pltpu.make_async_remote_copy(
            src_ref=src, dst_ref=dst, send_sem=ss, recv_sem=rs,
            device_id=(sp, tp), device_id_type=MESH,
        )

    def weight_copy(k):
        return pltpu.make_async_copy((qw, kw, vw)[k], WP.at[k], w_sem.at[k])

    def own_act():
        return pltpu.make_async_copy(act, A.at[t], own_sem.at[0])

    def own_ow():
        return pltpu.make_async_copy(ow, W.at[pl.ds(t * L, L)], own_sem.at[1])

    def act_across():
        return remote(act, A.at[t], a_send.at[0], a_recv.at[t], s, across)

    def act_mate():
        return remote(act, A.at[t], a_send.at[1], a_recv.at[t], s, mate)

    def act_pass():
        return remote(A.at[across], A.at[across], a_send.at[2], a_recv.at[across], s, mate)

    def wait_act(i):
        remote(act, A.at[i], a_send.at[0], a_recv.at[i], s, mate).wait_recv()

    def quarter(owner, q):
        rows = pl.ds(pl.multiple_of((q % 2) * (VALUE // 2), VALUE // 2), VALUE // 2)
        return owner * L + q // 2, rows

    def turn(j, row):
        return row * (2 * L - 1) if j == 0 else j

    def ow_across(j):
        q = turn(j, y)
        place, rows = quarter(t, q)
        return remote(
            ow.at[q // 2, rows], W.at[place, rows], o_send.at[j], o_recv.at[j], s, across
        )

    def ow_mate():
        return remote(ow, W.at[pl.ds(t * L, L)], m_send.at[0], m_recv.at[0], s, mate)

    last = 2 * L - 1

    def ow_beside():
        place, rows = quarter(across, turn(0, y))
        part = W.at[place, rows]
        return remote(part, part, o_send.at[last], o_recv.at[last], beside, t)

    def ow_pass(j):
        q = turn(0, 1 - y) if j == last else turn(j, y)
        place, rows = quarter(across, q)
        part = W.at[place, rows]
        return remote(part, part, m_send.at[1 + j], m_recv.at[1 + j], s, mate)

    def lam_out():
        return remote(LS, LB, lam_send.at[0], lam_recv.at[0], s, mate)

    for l in range(L):
        LS[l] = jnp.full((8, 128), lam_in[l], jnp.float32)
    act_across().start()
    act_mate().start()
    for k in range(3):
        weight_copy(k).start()
    own_act().start()
    for j in range(last):
        ow_across(j).start()
    own_ow().start()

    def piece_sp(l):
        return (c * L + l) * Y + y

    def piece(l, xx, d):
        return remote(
            PR.at[l, xx, d], PC.at[z, xx], p_send.at[l, xx, d], p_recv.at[z, xx],
            piece_sp(l), x * 2 + d,
        )

    def stays(l, d):
        return (piece_sp(l) == s) & (c == d)

    def send_piece(l, xx, d):
        @pl.when(stays(l, d))
        def _():
            pltpu.make_async_copy(PR.at[l, xx, d], PC.at[z, xx], p_recv.at[z, xx]).start()

        @pl.when(jnp.logical_not(stays(l, d)))
        def _():
            piece(l, xx, d).start()

    def project(xx):
        rows = A[pl.ds(xx * 2, 2)].reshape(2 * R, A.shape[2])
        for part in range(3):
            got = jnp.dot(rows, WP[part], preferred_element_type=jnp.float32)
            if part == 0:
                got = got * scale
            got = got.astype(jnp.bfloat16)
            for l in range(L):
                cols = got[:, l * 256:(l + 1) * 256]
                PR[l, xx, :, :, part * 256:(part + 1) * 256] = cols.reshape(2, R, 256)
        for i in range(L):
            l = upper * i + (1 - upper) * (L - 1 - i)
            for d in range(2):
                send_piece(l, xx, d)

    own_act().wait()
    for k in range(3):
        weight_copy(k).wait()
    wait_act(mate)
    project(x)
    ow_mate().start()
    lam_out().start()
    wait_act(across)
    act_pass().start()
    wait_act((1 - x) * 2 + (1 - c))
    project(1 - x)

    def kv_rows(row, zs, xx, core):
        return pl.ds(((zs * Y + row) * T + xx * 2 + core) * R, R)

    def kv_part(zs, xx):
        return PC.at[zs, xx, :, 256:768]

    def to_beside(zs, xx):
        return remote(
            kv_part(zs, xx), KV.at[kv_rows(y, zs, xx, c)],
            f_send.at[0, zs, xx], f_recv.at[0, zs, xx], beside, t,
        )

    def to_mate(zs, xx):
        return remote(
            kv_part(zs, xx), KV.at[kv_rows(y, zs, xx, c)],
            f_send.at[1, zs, xx], f_recv.at[1, zs, xx], s, mate,
        )

    def to_mate_again(zs, xx):
        part = KV.at[kv_rows(1 - y, zs, xx, c)]
        return remote(part, part, f_send.at[2, zs, xx], f_recv.at[2, zs, xx], s, mate)

    def to_self(zs, xx):
        return pltpu.make_async_copy(
            kv_part(zs, xx), KV.at[kv_rows(y, zs, xx, c)], f_recv.at[3, zs, xx]
        )

    def place(i):
        return (near + i // X) % Z, (x + i) % X

    def forward(i):
        zs, xx = place(i)
        remote(PR.at[0, 0, 0], PC.at[zs, xx], p_send.at[0, 0, 0], p_recv.at[zs, xx], s, mate).wait_recv()
        to_beside(zs, xx).start()
        to_mate(zs, xx).start()
        to_self(zs, xx).start()

    def relay(i):
        zs, xx = place(i)
        to_beside(zs, xx).wait_recv()
        to_mate_again(zs, xx).start()

    def spread(first, count):
        def both(i, carry):
            forward(first + i)

            @pl.when(i > 0)
            def _():
                relay(first + i - 1)

            return carry

        lax.fori_loop(0, count, both, 0)
        relay(first + count - 1)

    def wait_plane(zs):
        for xx in range(X):
            to_self(zs, xx).wait()
            to_mate(zs, xx).wait_recv()
            to_mate_again(zs, xx).wait_recv()

    q_rows = X * R
    k_rows = Y * span

    def chunk(i, j, masked):
        for m in range(2):
            q = PC[i, :, :, m * 128:(m + 1) * 128].reshape(q_rows, 128)
            keys = KV[pl.ds(j * k_rows, k_rows), m * 128:(m + 1) * 128]
            sc = lax.dot_general(
                q, keys, (((1,), (1,)), ((), ())), preferred_element_type=jnp.float32
            )
            if masked:
                row = lax.broadcasted_iota(jnp.int32, (q_rows, 1), 0)
                col = lax.broadcasted_iota(jnp.int32, (q_rows, k_rows), 1)
                pos = row + jnp.where(row >= R, R, 0) + (y * span + c * R)
                sc = jnp.where(col <= pos, sc, very_low)
            old = MX[i, m, :, :1]
            new = jnp.maximum(old, jnp.max(sc, axis=1, keepdims=True))
            p = jnp.exp2(sc - new)
            factor = jnp.exp2(old - new)
            total = DN[i, m, :, :1] * factor + jnp.sum(p, axis=1, keepdims=True)
            values = KV[pl.ds(j * k_rows, k_rows), 256:512]
            got = jnp.dot(p.astype(jnp.bfloat16), values, preferred_element_type=jnp.float32)
            ACC[i, m] = ACC[i, m] * factor + got
            MX[i, m] = jnp.broadcast_to(new, MX.shape[2:])
            DN[i, m] = jnp.broadcast_to(total, DN.shape[2:])

    def chunks(i, low, high, diagonal):
        def inner(j, carry):
            chunk(i, j, False)
            return carry

        lax.fori_loop(low, high, inner, 0)

        @pl.when(diagonal)
        def _():
            chunk(i, i, True)

    def home(zs, xx):
        return remote(
            HO.at[zs, xx], HI.at[head], h_send.at[zs, xx], h_recv.at[head],
            zs * Y + y, xx * 2 + c,
        )

    def ends_here(zs, xx):
        return (zs == z) & (xx == x)

    def finish(i):
        mine = jnp.where(z // L == c, LS[z % L], LB[z % L])[:1, :1]
        comb = ACC[i, 0] / DN[i, 0, :, :1] - mine * (ACC[i, 1] / DN[i, 1, :, :1])
        inv = lax.rsqrt(jnp.mean(comb * comb, axis=1, keepdims=True) + norm_floor)
        HO[i] = (comb * inv * gain[...]).astype(jnp.bfloat16).reshape(X, R, VALUE)
        for k in range(X):
            xx = (x + 1 + k) % X

            @pl.when(ends_here(i, xx))
            def _():
                pltpu.make_async_copy(HO.at[i, xx], HI.at[head], h_recv.at[head]).start()

            @pl.when(jnp.logical_not(ends_here(i, xx)))
            def _():
                home(i, xx).start()

    MX[...] = jnp.full(MX.shape, very_low, jnp.float32)
    DN[...] = jnp.zeros(DN.shape, jnp.float32)
    ACC[...] = jnp.zeros(ACC.shape, jnp.float32)
    H = Z // 2
    spread(0, H * X)
    ow_across(0).wait_recv()
    ow_beside().start()
    ow_pass(0).start()
    lam_out().wait_recv()
    for i in range(H):
        wait_plane(near + i)

    def step(k, carry):
        @pl.when(k == H)
        def _():
            spread(H * X, H * X)
            for i in range(H):
                wait_plane((near + H + i) % Z)
            for j in range(1, last - 1):
                ow_across(j).wait_recv()
                ow_pass(j).start()

        early = k < H
        i = jnp.where(early, near + k, jnp.where(upper == 1, k - H, Z - 1 - (k - H)))
        partial = (upper == 1) & (i >= H)
        low = jnp.where(early, near, 0)
        high = jnp.where(partial & jnp.logical_not(early), H, i)
        used = (upper == 1) | (k < Z)

        @pl.when(used)
        def _():
            chunks(i, low, high, jnp.logical_not(partial) | early)

            @pl.when(jnp.logical_not(partial & early))
            def _():
                finish(i)

        return carry

    lax.fori_loop(0, Z + H, step, 0)

    own_ow().wait()
    ow_mate().wait_recv()
    ow_across(last - 1).wait_recv()
    ow_pass(last - 1).start()
    ow_beside().wait_recv()
    ow_pass(last).start()
    TOT[...] = jnp.zeros(TOT.shape, jnp.float32)

    def add_head(i, carry):
        @pl.when(i == 2 * L)
        def _():
            for j in range(last + 1):
                ow_pass(j).wait_recv()

        h = (x * 2 * L + i) % (T * L)
        remote(HO.at[0, 0], HI.at[h], h_send.at[0, 0], h_recv.at[h], s, mate).wait_recv()
        TOT[...] += jnp.dot(HI[h], W[h], preferred_element_type=jnp.float32)
        return carry

    lax.fori_loop(0, T * L, add_head, 0)
    out[...] = TOT[...].astype(jnp.bfloat16)

    act_across().wait_send()
    act_mate().wait_send()
    act_pass().wait_send()
    ow_mate().wait_send()
    ow_beside().wait_send()
    for j in range(last):
        ow_across(j).wait_send()
    for j in range(last + 1):
        ow_pass(j).wait_send()
    lam_out().wait_send()
    for l in range(L):
        for xx in range(X):
            for d in range(2):
                @pl.when(jnp.logical_not(stays(l, d)))
                def _():
                    piece(l, xx, d).wait_send()

    def drain(zs, carry):
        for xx in range(X):
            to_beside(zs, xx).wait_send()
            to_mate(zs, xx).wait_send()
            to_mate_again(zs, xx).wait_send()

            @pl.when(jnp.logical_not(ends_here(zs, xx)))
            def _():
                home(zs, xx).wait_send()

        return carry

    lax.fori_loop(0, Z, drain, 0)


def fused(S, T, L, activations, query_weight, key_weight, value_weight, out_weight, lambdas, head_gain):
    R, D = activations.shape
    X, Y = 2, 2
    Z = S // Y
    bf, f32 = jnp.bfloat16, jnp.float32
    vmem = pl.BlockSpec(memory_space=pltpu.VMEM)
    hbm = pl.BlockSpec(memory_space=pl.ANY)
    smem = pl.BlockSpec(memory_space=pltpu.SMEM)
    dma = pltpu.SemaphoreType.DMA
    width = query_weight.shape[1]
    return pl.pallas_call(
        functools.partial(layer_kernel, S, T, L, R),
        out_shape=jax.ShapeDtypeStruct((R, D), bf),
        in_specs=[vmem, hbm, hbm, hbm, hbm, smem, vmem],
        out_specs=vmem,
        scratch_shapes=[
            pltpu.VMEM((T, R, D), bf),
            pltpu.VMEM((3, D, width), bf),
            pltpu.VMEM((T * L, VALUE, D), bf),
            pltpu.VMEM((L, X, 2, R, 768), bf),
            pltpu.VMEM((Z, X, R, 768), bf),
            pltpu.VMEM((S * T * R, 512), bf),
            pltpu.VMEM((Z, X, R, VALUE), bf),
            pltpu.VMEM((T * L, R, VALUE), bf),
            pltpu.VMEM((L, 8, 128), f32),
            pltpu.VMEM((L, 8, 128), f32),
            pltpu.VMEM((Z, 2, X * R, VALUE), f32),
            pltpu.VMEM((Z, 2, X * R, 128), f32),
            pltpu.VMEM((Z, 2, X * R, 128), f32),
            pltpu.VMEM((R, D), f32),
            dma((3,)), dma((2,)),
            dma((3,)), dma((T,)),
            dma((1,)), dma((1,)),
            dma((2 * L,)), dma((2 * L,)),
            dma((2 * L + 1,)), dma((2 * L + 1,)),
            dma((L, X, 2)), dma((Z, X)),
            dma((3, Z, X)), dma((4, Z, X)),
            dma((Z, X)), dma((T * L,)),
        ],
        compiler_params=pltpu.CompilerParams(
            has_side_effects=True, vmem_limit_bytes=60 * 1024 * 1024
        ),
    )(
        activations, query_weight, key_weight, value_weight,
        out_weight.reshape(L, VALUE, D), lambdas, head_gain.reshape(1, VALUE),
    )


def empty_state(count, local_heads):
    return (
        jnp.full((local_heads, 2, count), very_low, jnp.float32),
        jnp.zeros((local_heads, 2, count), jnp.float32),
        jnp.zeros((local_heads, 2, count, VALUE), jnp.float32),
    )


def absorb(state, query_set, query_pos, key_block, value_block, key_first):
    running, denoms, accums = state
    local_heads = running.shape[0]
    span = key_block.shape[0]
    key_grid = key_block.reshape(span, local_heads, 2, HEAD)
    scores = jnp.einsum(
        "qhme,khme->hmqk", query_set, key_grid, preferred_element_type=jnp.float32
    ) * HEAD ** (-0.5)
    key_pos = key_first + jnp.arange(span, dtype=jnp.int32)
    allowed = key_pos[None, :] <= query_pos[:, None]
    masked = jnp.where(allowed, scores, very_low)
    updated = jnp.maximum(running, jnp.max(masked, axis=-1))
    exp_weights = jnp.where(allowed, jnp.exp(masked - updated[..., None]), 0.0)
    factor = jnp.exp(running - updated)
    denoms = denoms * factor + jnp.sum(exp_weights, axis=-1)
    value_grid = value_block.reshape(span, local_heads, VALUE)
    product = jnp.einsum(
        "hmqk,khv->hmqv",
        exp_weights.astype(jnp.bfloat16),
        value_grid,
        preferred_element_type=jnp.float32,
    )
    accums = accums * factor[..., None] + product
    return (updated, denoms, accums)


def make_folder(query_sets, carry, pieces):
    key_piece, value_piece = pieces
    length = key_piece.shape[0]
    span = math.gcd(length, 512)

    def one_span(span_index, states):
        offset = span_index * span
        key_block = lax.dynamic_slice_in_dim(key_piece, offset, span, 0)
        value_block = lax.dynamic_slice_in_dim(value_piece, offset, span, 0)
        fresh = []
        for state, query_entry in zip(states, query_sets):
            query_set, query_pos = query_entry

            def take(current):
                return absorb(current, query_set, query_pos, key_block, value_block, offset)

            def leave(current):
                return current

            fresh.append(lax.cond(offset <= query_pos[-1], take, leave, state))
        return tuple(fresh)

    return lax.fori_loop(0, length // span, one_span, carry)


def shards(activations, query_weight, key_weight, value_weight, out_weight, lambdas, head_gain):
    local_heads = lambdas.shape[0]
    query_width = query_weight.shape[1]
    joined_weight = jnp.concatenate([query_weight, key_weight, value_weight], axis=1)
    projected = jnp.dot(
        lax.all_gather(activations, "tp", axis=0, tiled=True),
        joined_weight,
        preferred_element_type=jnp.float32,
    ).astype(jnp.bfloat16)
    row_count = projected.shape[0]
    queries = projected[:, :query_width].reshape(row_count, local_heads, 2, HEAD)
    key_rows = projected[:, query_width : 2 * query_width]
    value_rows = projected[:, 2 * query_width :]
    position = lax.axis_index("sp") * row_count + jnp.arange(row_count, dtype=jnp.int32)
    query_sets = [(queries, position)]
    start_states = tuple((empty_state(entry[0].shape[0], local_heads) for entry in query_sets))
    finals = make_folder(
        query_sets,
        start_states,
        (
            lax.all_gather(key_rows, "sp", axis=0, tiled=True),
            lax.all_gather(value_rows, "sp", axis=0, tiled=True),
        ),
    )
    outputs = []
    for state in finals:
        running, denoms, accums = state
        combined = (
            accums[:, 0] / denoms[:, 0, :, None]
            - lambdas[:, None, None] * accums[:, 1] / denoms[:, 1, :, None]
        )
        inverse_rms = lax.rsqrt(jnp.mean(combined * combined, axis=-1, keepdims=True) + norm_floor)
        normed = (combined * inverse_rms * head_gain).astype(jnp.bfloat16)
        outputs.append(
            jnp.transpose(normed, (1, 0, 2)).reshape(normed.shape[1], local_heads * VALUE)
        )
    heads_out = outputs[0]
    return lax.psum_scatter(
        jnp.dot(heads_out, out_weight, preferred_element_type=jnp.float32).astype(jnp.bfloat16),
        "tp",
        scatter_dimension=0,
        tiled=True,
    )


def solution(mesh):
    in_specs = (
        P(("sp", "tp"), None),
        P(None, "tp"),
        P(None, "tp"),
        P(None, "tp"),
        P("tp", None),
        P("tp"),
        P(),
    )
    out_specs = P(("sp", "tp"), None)
    S, T = mesh.shape["sp"], mesh.shape["tp"]

    def layer(*args):
        L = args[5].shape[0] // T
        rows = args[0].shape[0] // (S * T)
        fits = T == 4 and L == 2 and S == L * T and rows % 16 == 0
        local = functools.partial(fused, S, T, L) if fits else shards
        return jax.shard_map(
            local, mesh=mesh, in_specs=in_specs, out_specs=out_specs, check_vma=False
        )(*args)

    return layer
```

```python
import functools
import math

import jax
import jax.numpy as jnp
from jax import lax
from jax.experimental import pallas as pl
from jax.experimental.pallas import tpu as pltpu
from jax.sharding import PartitionSpec as P

HEAD = 128
VALUE = 256


norm_floor = 0.02
very_low = -1e30
MESH = pl.DeviceIdType.MESH


def layer_kernel(
    S, T, L, R,
    act, qw, kw, vw, ow, lam_in, gain,
    out,
    A, WP, W, PR, PC, KV, HO, HI, LS, LB, ACC, MX, DN, TOT,
    w_sem, own_sem, a_send, a_recv, lam_send, lam_recv, o_send, o_recv, m_send, m_recv,
    p_send, p_recv, f_send, f_recv, h_send, h_recv,
):
    X, Y = 2, 2
    Z = S // Y
    H = Z // 2
    s = lax.axis_index("sp")
    t = lax.axis_index("tp")
    x = t // 2
    c = t % 2
    y = s % Y
    z = s // Y
    mate = x * 2 + (1 - c)
    across = (1 - x) * 2 + c
    beside = z * Y + (1 - y)
    upper = z // (Z // 2)
    near = upper * (Z // 2)
    head = x * 2 * L + z
    span = T * R
    scale = HEAD ** (-0.5) * math.log2(math.e)

    def remote(src, dst, ss, rs, sp, tp):
        return pltpu.make_async_remote_copy(
            src_ref=src, dst_ref=dst, send_sem=ss, recv_sem=rs,
            device_id=(sp, tp), device_id_type=MESH,
        )

    def weight_copy(k):
        return pltpu.make_async_copy((qw, kw, vw)[k], WP.at[k], w_sem.at[k])

    def own_act():
        return pltpu.make_async_copy(act, A.at[t], own_sem.at[0])

    def own_ow():
        return pltpu.make_async_copy(ow, W.at[pl.ds(t * L, L)], own_sem.at[1])

    def act_across():
        return remote(act, A.at[t], a_send.at[0], a_recv.at[t], s, across)

    def act_mate():
        return remote(act, A.at[t], a_send.at[1], a_recv.at[t], s, mate)

    def act_pass():
        return remote(A.at[across], A.at[across], a_send.at[2], a_recv.at[across], s, mate)

    def wait_act(i):
        remote(act, A.at[i], a_send.at[0], a_recv.at[i], s, mate).wait_recv()

    def quarter(owner, q):
        rows = pl.ds(pl.multiple_of((q % 2) * (VALUE // 2), VALUE // 2), VALUE // 2)
        return owner * L + q // 2, rows

    def turn(j, row):
        return row * (2 * L - 1) if j == 0 else j

    def ow_across(j):
        q = turn(j, y)
        place, rows = quarter(t, q)
        return remote(
            ow.at[q // 2, rows], W.at[place, rows], o_send.at[j], o_recv.at[j], s, across
        )

    def ow_mate():
        return remote(ow, W.at[pl.ds(t * L, L)], m_send.at[0], m_recv.at[0], s, mate)

    last = 2 * L - 1

    cut = VALUE // 2 // (H * X)

    def ow_beside(k, row):
        q = turn(0, row)
        first = pl.multiple_of((q % 2) * (VALUE // 2) + k * cut, cut)
        part = W.at[across * L + q // 2, pl.ds(first, cut)]
        return remote(part, part, o_send.at[last + k], o_recv.at[last + k], beside, t)

    def ow_pass(j):
        q = turn(0, 1 - y) if j == last else turn(j, y)
        place, rows = quarter(across, q)
        part = W.at[place, rows]
        return remote(part, part, m_send.at[1 + j], m_recv.at[1 + j], s, mate)

    def lam_out():
        return remote(LS, LB, lam_send.at[0], lam_recv.at[0], s, mate)

    barrier = pltpu.get_barrier_semaphore()
    greeted = [(beside, t)]
    for i in range(Z):
        row = ((z + i) % Z) * Y + y
        greeted += [(row, mate), (row, across)] + ([(row, t)] if i > 0 else [])
    for sp, tp in greeted:
        pl.semaphore_signal(barrier, inc=1, device_id=(sp, tp), device_id_type=MESH)
    weight_copies = [weight_copy(k) for k in range(3)]
    for copy in weight_copies:
        copy.start()
    own_act().start()
    own_ow().start()
    pl.semaphore_wait(barrier, len(greeted))

    for l in range(L):
        LS[l] = jnp.full((8, 128), lam_in[l], jnp.float32)
    act_across().start()
    act_mate().start()
    for j in range(last):
        ow_across(j).start()

    def piece_sp(l):
        return (c * L + l) * Y + y

    def piece(l, xx, d):
        return remote(
            PR.at[l, xx, d], PC.at[z, xx], p_send.at[l, xx, d], p_recv.at[z, xx],
            piece_sp(l), x * 2 + d,
        )

    def stays(l, d):
        return (piece_sp(l) == s) & (c == d)

    def send_piece(l, xx, d):
        @pl.when(stays(l, d))
        def _():
            pltpu.make_async_copy(PR.at[l, xx, d], PC.at[z, xx], p_recv.at[z, xx]).start()

        @pl.when(jnp.logical_not(stays(l, d)))
        def _():
            piece(l, xx, d).start()

    def project(xx):
        rows = A[pl.ds(xx * 2, 2)].reshape(2 * R, A.shape[2])
        for part in range(3):
            got = jnp.dot(rows, WP[part], preferred_element_type=jnp.float32)
            if part == 0:
                got = got * scale
            got = got.astype(jnp.bfloat16)
            for l in range(L):
                cols = got[:, l * 256:(l + 1) * 256]
                PR[l, xx, :, :, part * 256:(part + 1) * 256] = cols.reshape(2, R, 256)
        for i in range(L):
            l = upper * i + (1 - upper) * (L - 1 - i)
            for d in range(2):
                send_piece(l, xx, d)

    own_act().wait()
    for k in range(3):
        weight_copy(k).wait()
    wait_act(mate)
    project(x)
    lam_out().start()
    wait_act(across)
    act_pass().start()
    wait_act((1 - x) * 2 + (1 - c))
    project(1 - x)

    def kv_rows(row, zs, xx, core):
        return pl.ds(((zs * Y + row) * T + xx * 2 + core) * R, R)

    def kv_part(zs, xx):
        return PC.at[zs, xx, :, 256:768]

    def to_beside(zs, xx):
        return remote(
            kv_part(zs, xx), KV.at[kv_rows(y, zs, xx, c)],
            f_send.at[0, zs, xx], f_recv.at[0, zs, xx], beside, t,
        )

    def to_mate(zs, xx):
        return remote(
            kv_part(zs, xx), KV.at[kv_rows(y, zs, xx, c)],
            f_send.at[1, zs, xx], f_recv.at[1, zs, xx], s, mate,
        )

    def to_mate_again(zs, xx):
        part = KV.at[kv_rows(1 - y, zs, xx, c)]
        return remote(part, part, f_send.at[2, zs, xx], f_recv.at[2, zs, xx], s, mate)

    def to_self(zs, xx):
        return pltpu.make_async_copy(
            kv_part(zs, xx), KV.at[kv_rows(y, zs, xx, c)], f_recv.at[3, zs, xx]
        )

    def place(i):
        return (near + i // X) % Z, (x + i) % X

    def forward(i):
        zs, xx = place(i)
        remote(PR.at[0, 0, 0], PC.at[zs, xx], p_send.at[0, 0, 0], p_recv.at[zs, xx], s, mate).wait_recv()
        to_beside(zs, xx).start()
        to_mate(zs, xx).start()
        to_self(zs, xx).start()

    def relay(i):
        zs, xx = place(i)
        to_beside(zs, xx).wait_recv()
        to_mate_again(zs, xx).start()

    def spread(first, count, weights):
        def both(i, carry):
            forward(first + i)
            if weights:
                ow_beside(i, y).start()

            @pl.when(i > 0)
            def _():
                relay(first + i - 1)

            return carry

        lax.fori_loop(0, count, both, 0)
        relay(first + count - 1)

    def wait_plane(zs):
        for xx in range(X):
            to_self(zs, xx).wait()
            to_mate(zs, xx).wait_recv()
            to_mate_again(zs, xx).wait_recv()

    q_rows = X * R
    k_rows = Y * span

    def chunk(i, j, masked):
        for m in range(2):
            q = PC[i, :, :, m * 128:(m + 1) * 128].reshape(q_rows, 128)
            keys = KV[pl.ds(j * k_rows, k_rows), m * 128:(m + 1) * 128]
            sc = lax.dot_general(
                q, keys, (((1,), (1,)), ((), ())), preferred_element_type=jnp.float32
            )
            if masked:
                row = lax.broadcasted_iota(jnp.int32, (q_rows, 1), 0)
                col = lax.broadcasted_iota(jnp.int32, (q_rows, k_rows), 1)
                pos = row + jnp.where(row >= R, R, 0) + (y * span + c * R)
                sc = jnp.where(col <= pos, sc, very_low)
            old = MX[i, m, :, :1]
            new = jnp.maximum(old, jnp.max(sc, axis=1, keepdims=True))
            p = jnp.exp2(sc - new)
            factor = jnp.exp2(old - new)
            total = DN[i, m, :, :1] * factor + jnp.sum(p, axis=1, keepdims=True)
            values = KV[pl.ds(j * k_rows, k_rows), 256:512]
            got = jnp.dot(p.astype(jnp.bfloat16), values, preferred_element_type=jnp.float32)
            ACC[i, m] = ACC[i, m] * factor + got
            MX[i, m] = jnp.broadcast_to(new, MX.shape[2:])
            DN[i, m] = jnp.broadcast_to(total, DN.shape[2:])

    def chunks(i, low, high, diagonal):
        def inner(j, carry):
            chunk(i, j, False)
            return carry

        lax.fori_loop(low, high, inner, 0)

        @pl.when(diagonal)
        def _():
            chunk(i, i, True)

    def home(zs, xx):
        return remote(
            HO.at[zs, xx], HI.at[head], h_send.at[zs, xx], h_recv.at[head],
            zs * Y + y, xx * 2 + c,
        )

    def ends_here(zs, xx):
        return (zs == z) & (xx == x)

    def finish(i):
        mine = jnp.where(z // L == c, LS[z % L], LB[z % L])[:1, :1]
        comb = ACC[i, 0] / DN[i, 0, :, :1] - mine * (ACC[i, 1] / DN[i, 1, :, :1])
        inv = lax.rsqrt(jnp.mean(comb * comb, axis=1, keepdims=True) + norm_floor)
        HO[i] = (comb * inv * gain[...]).astype(jnp.bfloat16).reshape(X, R, VALUE)
        for k in range(X):
            xx = (x + 1 + k) % X

            @pl.when(ends_here(i, xx))
            def _():
                pltpu.make_async_copy(HO.at[i, xx], HI.at[head], h_recv.at[head]).start()

            @pl.when(jnp.logical_not(ends_here(i, xx)))
            def _():
                home(i, xx).start()

    MX[...] = jnp.full(MX.shape, very_low, jnp.float32)
    DN[...] = jnp.zeros(DN.shape, jnp.float32)
    ACC[...] = jnp.zeros(ACC.shape, jnp.float32)
    spread(0, H * X, False)
    lam_out().wait_recv()
    for i in range(H):
        wait_plane(near + i)

    def step(k, carry):
        @pl.when(k == H)
        def _():
            ow_across(0).wait_recv()
            spread(H * X, H * X, True)
            ow_mate().start()
            ow_pass(0).start()
            for i in range(H):
                wait_plane((near + H + i) % Z)
            for j in range(1, last - 1):
                ow_across(j).wait_recv()
                ow_pass(j).start()

        @pl.when(k == Z - 1)
        def _():
            ow_across(last - 1).wait_recv()
            ow_pass(last - 1).start()
            for i in range(H * X):
                ow_beside(i, 1 - y).wait_recv()
            ow_pass(last).start()

        early = k < H
        i = jnp.where(early, near + k, jnp.where(upper == 1, k - H, Z - 1 - (k - H)))
        partial = (upper == 1) & (i >= H)
        low = jnp.where(early, near, 0)
        high = jnp.where(partial & jnp.logical_not(early), H, i)
        used = (upper == 1) | (k < Z)

        @pl.when(used)
        def _():
            chunks(i, low, high, jnp.logical_not(partial) | early)

            @pl.when(jnp.logical_not(partial & early))
            def _():
                finish(i)

        return carry

    lax.fori_loop(0, Z + H, step, 0)

    own_ow().wait()
    ow_mate().wait_recv()
    TOT[...] = jnp.zeros(TOT.shape, jnp.float32)

    def add_head(i, carry):
        @pl.when(i == 2 * L)
        def _():
            for j in range(last + 1):
                ow_pass(j).wait_recv()

        h = (x * 2 * L + i) % (T * L)
        remote(HO.at[0, 0], HI.at[h], h_send.at[0, 0], h_recv.at[h], s, mate).wait_recv()
        TOT[...] += jnp.dot(HI[h], W[h], preferred_element_type=jnp.float32)
        return carry

    lax.fori_loop(0, T * L, add_head, 0)
    out[...] = TOT[...].astype(jnp.bfloat16)

    act_across().wait_send()
    act_mate().wait_send()
    act_pass().wait_send()
    ow_mate().wait_send()
    for i in range(H * X):
        ow_beside(i, y).wait_send()
    for j in range(last):
        ow_across(j).wait_send()
    for j in range(last + 1):
        ow_pass(j).wait_send()
    lam_out().wait_send()
    for l in range(L):
        for xx in range(X):
            for d in range(2):
                @pl.when(jnp.logical_not(stays(l, d)))
                def _():
                    piece(l, xx, d).wait_send()

    def drain(zs, carry):
        for xx in range(X):
            to_beside(zs, xx).wait_send()
            to_mate(zs, xx).wait_send()
            to_mate_again(zs, xx).wait_send()

            @pl.when(jnp.logical_not(ends_here(zs, xx)))
            def _():
                home(zs, xx).wait_send()

        return carry

    lax.fori_loop(0, Z, drain, 0)


def fused(S, T, L, activations, query_weight, key_weight, value_weight, out_weight, lambdas, head_gain):
    R, D = activations.shape
    X, Y = 2, 2
    Z = S // Y
    bf, f32 = jnp.bfloat16, jnp.float32
    vmem = pl.BlockSpec(memory_space=pltpu.VMEM)
    hbm = pl.BlockSpec(memory_space=pl.ANY)
    smem = pl.BlockSpec(memory_space=pltpu.SMEM)
    dma = pltpu.SemaphoreType.DMA
    width = query_weight.shape[1]
    return pl.pallas_call(
        functools.partial(layer_kernel, S, T, L, R),
        out_shape=jax.ShapeDtypeStruct((R, D), bf),
        in_specs=[vmem, hbm, hbm, hbm, hbm, smem, vmem],
        out_specs=vmem,
        scratch_shapes=[
            pltpu.VMEM((T, R, D), bf),
            pltpu.VMEM((3, D, width), bf),
            pltpu.VMEM((T * L, VALUE, D), bf),
            pltpu.VMEM((L, X, 2, R, 768), bf),
            pltpu.VMEM((Z, X, R, 768), bf),
            pltpu.VMEM((S * T * R, 512), bf),
            pltpu.VMEM((Z, X, R, VALUE), bf),
            pltpu.VMEM((T * L, R, VALUE), bf),
            pltpu.VMEM((L, 8, 128), f32),
            pltpu.VMEM((L, 8, 128), f32),
            pltpu.VMEM((Z, 2, X * R, VALUE), f32),
            pltpu.VMEM((Z, 2, X * R, 128), f32),
            pltpu.VMEM((Z, 2, X * R, 128), f32),
            pltpu.VMEM((R, D), f32),
            dma((3,)), dma((2,)),
            dma((3,)), dma((T,)),
            dma((1,)), dma((1,)),
            dma((2 * L - 1 + Z // 2 * X,)), dma((2 * L - 1 + Z // 2 * X,)),
            dma((2 * L + 1,)), dma((2 * L + 1,)),
            dma((L, X, 2)), dma((Z, X)),
            dma((3, Z, X)), dma((4, Z, X)),
            dma((Z, X)), dma((T * L,)),
        ],
        compiler_params=pltpu.CompilerParams(
            has_side_effects=True, collective_id=0, vmem_limit_bytes=60 * 1024 * 1024
        ),
    )(
        activations, query_weight, key_weight, value_weight,
        out_weight.reshape(L, VALUE, D), lambdas, head_gain.reshape(1, VALUE),
    )


def empty_state(count, local_heads):
    return (
        jnp.full((local_heads, 2, count), very_low, jnp.float32),
        jnp.zeros((local_heads, 2, count), jnp.float32),
        jnp.zeros((local_heads, 2, count, VALUE), jnp.float32),
    )


def absorb(state, query_set, query_pos, key_block, value_block, key_first):
    running, denoms, accums = state
    local_heads = running.shape[0]
    span = key_block.shape[0]
    key_grid = key_block.reshape(span, local_heads, 2, HEAD)
    scores = jnp.einsum(
        "qhme,khme->hmqk", query_set, key_grid, preferred_element_type=jnp.float32
    ) * HEAD ** (-0.5)
    key_pos = key_first + jnp.arange(span, dtype=jnp.int32)
    allowed = key_pos[None, :] <= query_pos[:, None]
    masked = jnp.where(allowed, scores, very_low)
    updated = jnp.maximum(running, jnp.max(masked, axis=-1))
    exp_weights = jnp.where(allowed, jnp.exp(masked - updated[..., None]), 0.0)
    factor = jnp.exp(running - updated)
    denoms = denoms * factor + jnp.sum(exp_weights, axis=-1)
    value_grid = value_block.reshape(span, local_heads, VALUE)
    product = jnp.einsum(
        "hmqk,khv->hmqv",
        exp_weights.astype(jnp.bfloat16),
        value_grid,
        preferred_element_type=jnp.float32,
    )
    accums = accums * factor[..., None] + product
    return (updated, denoms, accums)


def make_folder(query_sets, carry, pieces):
    key_piece, value_piece = pieces
    length = key_piece.shape[0]
    span = math.gcd(length, 512)

    def one_span(span_index, states):
        offset = span_index * span
        key_block = lax.dynamic_slice_in_dim(key_piece, offset, span, 0)
        value_block = lax.dynamic_slice_in_dim(value_piece, offset, span, 0)
        fresh = []
        for state, query_entry in zip(states, query_sets):
            query_set, query_pos = query_entry

            def take(current):
                return absorb(current, query_set, query_pos, key_block, value_block, offset)

            def leave(current):
                return current

            fresh.append(lax.cond(offset <= query_pos[-1], take, leave, state))
        return tuple(fresh)

    return lax.fori_loop(0, length // span, one_span, carry)


def shards(activations, query_weight, key_weight, value_weight, out_weight, lambdas, head_gain):
    local_heads = lambdas.shape[0]
    query_width = query_weight.shape[1]
    joined_weight = jnp.concatenate([query_weight, key_weight, value_weight], axis=1)
    projected = jnp.dot(
        lax.all_gather(activations, "tp", axis=0, tiled=True),
        joined_weight,
        preferred_element_type=jnp.float32,
    ).astype(jnp.bfloat16)
    row_count = projected.shape[0]
    queries = projected[:, :query_width].reshape(row_count, local_heads, 2, HEAD)
    key_rows = projected[:, query_width : 2 * query_width]
    value_rows = projected[:, 2 * query_width :]
    position = lax.axis_index("sp") * row_count + jnp.arange(row_count, dtype=jnp.int32)
    query_sets = [(queries, position)]
    start_states = tuple((empty_state(entry[0].shape[0], local_heads) for entry in query_sets))
    finals = make_folder(
        query_sets,
        start_states,
        (
            lax.all_gather(key_rows, "sp", axis=0, tiled=True),
            lax.all_gather(value_rows, "sp", axis=0, tiled=True),
        ),
    )
    outputs = []
    for state in finals:
        running, denoms, accums = state
        combined = (
            accums[:, 0] / denoms[:, 0, :, None]
            - lambdas[:, None, None] * accums[:, 1] / denoms[:, 1, :, None]
        )
        inverse_rms = lax.rsqrt(jnp.mean(combined * combined, axis=-1, keepdims=True) + norm_floor)
        normed = (combined * inverse_rms * head_gain).astype(jnp.bfloat16)
        outputs.append(
            jnp.transpose(normed, (1, 0, 2)).reshape(normed.shape[1], local_heads * VALUE)
        )
    heads_out = outputs[0]
    return lax.psum_scatter(
        jnp.dot(heads_out, out_weight, preferred_element_type=jnp.float32).astype(jnp.bfloat16),
        "tp",
        scatter_dimension=0,
        tiled=True,
    )


def solution(mesh):
    in_specs = (
        P(("sp", "tp"), None),
        P(None, "tp"),
        P(None, "tp"),
        P(None, "tp"),
        P("tp", None),
        P("tp"),
        P(),
    )
    out_specs = P(("sp", "tp"), None)
    S, T = mesh.shape["sp"], mesh.shape["tp"]

    def layer(*args):
        L = args[5].shape[0] // T
        rows = args[0].shape[0] // (S * T)
        fits = T == 4 and L == 2 and S == L * T and rows % 16 == 0
        local = functools.partial(fused, S, T, L) if fits else shards
        return jax.shard_map(
            local, mesh=mesh, in_specs=in_specs, out_specs=out_specs, check_vma=False
        )(*args)

    return layer
```

```python
import functools
import math

import jax
import jax.numpy as jnp
from jax import lax
from jax.experimental import pallas as pl
from jax.experimental.pallas import tpu as pltpu
from jax.sharding import PartitionSpec as P

HEAD = 128
VALUE = 256


norm_floor = 0.02
very_low = -1e30
MESH = pl.DeviceIdType.MESH


def layer_kernel(
    S, T, L, R,
    act, qw, kw, vw, ow, lam_in, gain,
    out,
    A, WP, W, PR, PC, KV, HO, HI, LS, LB, ACC, MX, DN, TOT,
    w_sem, own_sem, a_send, a_recv, lam_send, lam_recv, o_send, o_recv, m_send, m_recv,
    p_send, p_recv, f_send, f_recv, h_send, h_recv,
):
    X, Y = 2, 2
    Z = S // Y
    H = Z // 2
    s = lax.axis_index("sp")
    t = lax.axis_index("tp")
    x = t // 2
    c = t % 2
    y = s % Y
    z = s // Y
    mate = x * 2 + (1 - c)
    across = (1 - x) * 2 + c
    beside = z * Y + (1 - y)
    upper = z // (Z // 2)
    near = upper * (Z // 2)
    head = x * 2 * L + z
    span = T * R
    scale = HEAD ** (-0.5) * math.log2(math.e)

    def remote(src, dst, ss, rs, sp, tp):
        return pltpu.make_async_remote_copy(
            src_ref=src, dst_ref=dst, send_sem=ss, recv_sem=rs,
            device_id=(sp, tp), device_id_type=MESH,
        )

    def weight_copy(k):
        return pltpu.make_async_copy((qw, kw, vw)[k], WP.at[k], w_sem.at[k])

    def own_act():
        return pltpu.make_async_copy(act, A.at[t], own_sem.at[0])

    def own_ow():
        return pltpu.make_async_copy(ow, W.at[pl.ds(t * L, L)], own_sem.at[1])

    def act_across():
        return remote(act, A.at[t], a_send.at[0], a_recv.at[t], s, across)

    def act_mate():
        return remote(act, A.at[t], a_send.at[1], a_recv.at[t], s, mate)

    def act_pass():
        return remote(A.at[across], A.at[across], a_send.at[2], a_recv.at[across], s, mate)

    def wait_act(i):
        remote(act, A.at[i], a_send.at[0], a_recv.at[i], s, mate).wait_recv()

    def quarter(owner, q):
        rows = pl.ds(pl.multiple_of((q % 2) * (VALUE // 2), VALUE // 2), VALUE // 2)
        return owner * L + q // 2, rows

    def turn(j, row):
        return row * (2 * L - 1) if j == 0 else j

    def ow_across(j):
        q = turn(j, y)
        place, rows = quarter(t, q)
        return remote(
            ow.at[q // 2, rows], W.at[place, rows], o_send.at[j], o_recv.at[j], s, across
        )

    def ow_mate():
        return remote(ow, W.at[pl.ds(t * L, L)], m_send.at[0], m_recv.at[0], s, mate)

    last = 2 * L - 1

    cut = VALUE // 2 // H

    def ow_beside(k, row):
        q = turn(0, row)
        first = pl.multiple_of((q % 2) * (VALUE // 2) + k * cut, cut)
        part = W.at[across * L + q // 2, pl.ds(first, cut)]
        return remote(part, part, o_send.at[last + k], o_recv.at[last + k], beside, t)

    def ow_pass(j):
        q = turn(0, 1 - y) if j == last else turn(j, y)
        place, rows = quarter(across, q)
        part = W.at[place, rows]
        return remote(part, part, m_send.at[1 + j], m_recv.at[1 + j], s, mate)

    def lam_out():
        return remote(LS, LB, lam_send.at[0], lam_recv.at[0], s, mate)

    barrier = pltpu.get_barrier_semaphore()
    greeted = [(beside, t)]
    for i in range(Z):
        row = ((z + i) % Z) * Y + y
        greeted += [(row, mate), (row, across)] + ([(row, t)] if i > 0 else [])
    for sp, tp in greeted:
        pl.semaphore_signal(barrier, inc=1, device_id=(sp, tp), device_id_type=MESH)
    weight_copies = [weight_copy(k) for k in range(3)]
    for copy in weight_copies:
        copy.start()
    own_act().start()
    own_ow().start()
    pl.semaphore_wait(barrier, len(greeted))

    for l in range(L):
        LS[l] = jnp.full((8, 128), lam_in[l], jnp.float32)
    act_across().start()
    act_mate().start()
    for j in range(last):
        ow_across(j).start()

    def piece_sp(l):
        return (c * L + l) * Y + y

    def piece(l, xx, d):
        return remote(
            PR.at[l, xx, d], PC.at[z, xx], p_send.at[l, xx, d], p_recv.at[z, xx],
            piece_sp(l), x * 2 + d,
        )

    def stays(l, d):
        return (piece_sp(l) == s) & (c == d)

    def send_piece(l, xx, d):
        @pl.when(stays(l, d))
        def _():
            pltpu.make_async_copy(PR.at[l, xx, d], PC.at[z, xx], p_recv.at[z, xx]).start()

        @pl.when(jnp.logical_not(stays(l, d)))
        def _():
            piece(l, xx, d).start()

    def project(xx):
        rows = A[pl.ds(xx * 2, 2)].reshape(2 * R, A.shape[2])
        for part in range(3):
            got = jnp.dot(rows, WP[part], preferred_element_type=jnp.float32)
            if part == 0:
                got = got * scale
            got = got.astype(jnp.bfloat16)
            for l in range(L):
                cols = got[:, l * 256:(l + 1) * 256]
                PR[l, xx, :, :, part * 256:(part + 1) * 256] = cols.reshape(2, R, 256)
        for i in range(L):
            l = upper * i + (1 - upper) * (L - 1 - i)
            for d in range(2):
                send_piece(l, xx, d)

    own_act().wait()
    for k in range(3):
        weight_copy(k).wait()
    wait_act(mate)
    project(x)
    lam_out().start()
    wait_act(across)
    act_pass().start()
    wait_act((1 - x) * 2 + (1 - c))
    project(1 - x)

    def kv_rows(row, zs, xx, core):
        return pl.ds(((zs * Y + row) * T + xx * 2 + core) * R, R)

    def kv_part(zs, xx):
        return PC.at[zs, xx, :, 256:768]

    def to_beside(zs, xx):
        return remote(
            kv_part(zs, xx), KV.at[kv_rows(y, zs, xx, c)],
            f_send.at[0, zs, xx], f_recv.at[0, zs, xx], beside, t,
        )

    def to_mate(zs, xx):
        return remote(
            kv_part(zs, xx), KV.at[kv_rows(y, zs, xx, c)],
            f_send.at[1, zs, xx], f_recv.at[1, zs, xx], s, mate,
        )

    def to_mate_again(zs, xx):
        part = KV.at[kv_rows(1 - y, zs, xx, c)]
        return remote(part, part, f_send.at[2, zs, xx], f_recv.at[2, zs, xx], s, mate)

    def to_self(zs, xx):
        return pltpu.make_async_copy(
            kv_part(zs, xx), KV.at[kv_rows(y, zs, xx, c)], f_recv.at[3, zs, xx]
        )

    def place(i):
        return (near + i) % Z, (x + i // Z) % X

    def forward(i):
        zs, xx = place(i)
        remote(PR.at[0, 0, 0], PC.at[zs, xx], p_send.at[0, 0, 0], p_recv.at[zs, xx], s, mate).wait_recv()
        to_beside(zs, xx).start()
        to_mate(zs, xx).start()
        to_self(zs, xx).start()

    def relay(i):
        zs, xx = place(i)
        to_beside(zs, xx).wait_recv()
        to_mate_again(zs, xx).start()

    def spread(first, count, weights):
        def both(i, carry):
            forward(first + i)
            if weights:
                @pl.when(i == 0)
                def _():
                    ow_across(0).wait_recv()

                ow_beside(i, y).start()

            @pl.when(i > 0)
            def _():
                relay(first + i - 1)

            return carry

        lax.fori_loop(0, count, both, 0)
        relay(first + count - 1)

    def wait_plane(zs):
        for xx in range(X):
            to_self(zs, xx).wait()
            to_mate(zs, xx).wait_recv()
            to_mate_again(zs, xx).wait_recv()

    q_rows = X * R
    k_rows = Y * span

    def chunk(i, j, masked):
        for m in range(2):
            q = PC[i, :, :, m * 128:(m + 1) * 128].reshape(q_rows, 128)
            keys = KV[pl.ds(j * k_rows, k_rows), m * 128:(m + 1) * 128]
            sc = lax.dot_general(
                q, keys, (((1,), (1,)), ((), ())), preferred_element_type=jnp.float32
            )
            if masked:
                row = lax.broadcasted_iota(jnp.int32, (q_rows, 1), 0)
                col = lax.broadcasted_iota(jnp.int32, (q_rows, k_rows), 1)
                pos = row + jnp.where(row >= R, R, 0) + (y * span + c * R)
                sc = jnp.where(col <= pos, sc, very_low)
            old = MX[i, m, :, :1]
            new = jnp.maximum(old, jnp.max(sc, axis=1, keepdims=True))
            p = jnp.exp2(sc - new)
            factor = jnp.exp2(old - new)
            total = DN[i, m, :, :1] * factor + jnp.sum(p, axis=1, keepdims=True)
            values = KV[pl.ds(j * k_rows, k_rows), 256:512]
            got = jnp.dot(p.astype(jnp.bfloat16), values, preferred_element_type=jnp.float32)
            ACC[i, m] = ACC[i, m] * factor + got
            MX[i, m] = jnp.broadcast_to(new, MX.shape[2:])
            DN[i, m] = jnp.broadcast_to(total, DN.shape[2:])

    def chunks(i, low, high, diagonal):
        def inner(j, carry):
            chunk(i, j, False)
            return carry

        lax.fori_loop(low, high, inner, 0)

        @pl.when(diagonal)
        def _():
            chunk(i, i, True)

    def home(zs, xx):
        return remote(
            HO.at[zs, xx], HI.at[head], h_send.at[zs, xx], h_recv.at[head],
            zs * Y + y, xx * 2 + c,
        )

    def ends_here(zs, xx):
        return (zs == z) & (xx == x)

    def finish(i):
        mine = jnp.where(z // L == c, LS[z % L], LB[z % L])[:1, :1]
        comb = ACC[i, 0] / DN[i, 0, :, :1] - mine * (ACC[i, 1] / DN[i, 1, :, :1])
        inv = lax.rsqrt(jnp.mean(comb * comb, axis=1, keepdims=True) + norm_floor)
        HO[i] = (comb * inv * gain[...]).astype(jnp.bfloat16).reshape(X, R, VALUE)
        for k in range(X):
            xx = (x + 1 + k) % X

            @pl.when(ends_here(i, xx))
            def _():
                pltpu.make_async_copy(HO.at[i, xx], HI.at[head], h_recv.at[head]).start()

            @pl.when(jnp.logical_not(ends_here(i, xx)))
            def _():
                home(i, xx).start()

    MX[...] = jnp.full(MX.shape, very_low, jnp.float32)
    DN[...] = jnp.zeros(DN.shape, jnp.float32)
    ACC[...] = jnp.zeros(ACC.shape, jnp.float32)
    spread(0, Z + H, False)
    lam_out().wait_recv()
    for i in range(H):
        wait_plane(near + i)

    def step(k, carry):
        @pl.when(k == H)
        def _():
            spread(Z + H, H, True)
            ow_mate().start()
            for i in range(H):
                wait_plane((near + H + i) % Z)

        @pl.when(k == Z - 1)
        def _():
            ow_pass(0).start()
            for j in range(1, last - 1):
                ow_across(j).wait_recv()
                ow_pass(j).start()

        early = k < H
        i = jnp.where(early, near + k, jnp.where(upper == 1, k - H, Z - 1 - (k - H)))
        partial = (upper == 1) & (i >= H)
        low = jnp.where(early, near, 0)
        high = jnp.where(partial & jnp.logical_not(early), H, i)
        used = (upper == 1) | (k < Z)

        @pl.when(used)
        def _():
            chunks(i, low, high, jnp.logical_not(partial) | early)

            @pl.when(jnp.logical_not(partial & early))
            def _():
                finish(i)

        return carry

    lax.fori_loop(0, Z + H, step, 0)

    own_ow().wait()
    ow_mate().wait_recv()
    for i in range(H):
        ow_beside(i, 1 - y).wait_recv()
    ow_pass(last).start()
    ow_across(last - 1).wait_recv()
    ow_pass(last - 1).start()
    TOT[...] = jnp.zeros(TOT.shape, jnp.float32)

    def add_head(i, carry):
        @pl.when(i == 2 * L)
        def _():
            for j in range(last + 1):
                ow_pass(j).wait_recv()

        h = (x * 2 * L + i) % (T * L)
        remote(HO.at[0, 0], HI.at[h], h_send.at[0, 0], h_recv.at[h], s, mate).wait_recv()
        TOT[...] += jnp.dot(HI[h], W[h], preferred_element_type=jnp.float32)
        return carry

    lax.fori_loop(0, T * L, add_head, 0)
    out[...] = TOT[...].astype(jnp.bfloat16)

    act_across().wait_send()
    act_mate().wait_send()
    act_pass().wait_send()
    ow_mate().wait_send()
    for i in range(H):
        ow_beside(i, y).wait_send()
    for j in range(last):
        ow_across(j).wait_send()
    for j in range(last + 1):
        ow_pass(j).wait_send()
    lam_out().wait_send()
    for l in range(L):
        for xx in range(X):
            for d in range(2):
                @pl.when(jnp.logical_not(stays(l, d)))
                def _():
                    piece(l, xx, d).wait_send()

    def drain(zs, carry):
        for xx in range(X):
            to_beside(zs, xx).wait_send()
            to_mate(zs, xx).wait_send()
            to_mate_again(zs, xx).wait_send()

            @pl.when(jnp.logical_not(ends_here(zs, xx)))
            def _():
                home(zs, xx).wait_send()

        return carry

    lax.fori_loop(0, Z, drain, 0)


def fused(S, T, L, activations, query_weight, key_weight, value_weight, out_weight, lambdas, head_gain):
    R, D = activations.shape
    X, Y = 2, 2
    Z = S // Y
    bf, f32 = jnp.bfloat16, jnp.float32
    vmem = pl.BlockSpec(memory_space=pltpu.VMEM)
    hbm = pl.BlockSpec(memory_space=pl.ANY)
    smem = pl.BlockSpec(memory_space=pltpu.SMEM)
    dma = pltpu.SemaphoreType.DMA
    width = query_weight.shape[1]
    return pl.pallas_call(
        functools.partial(layer_kernel, S, T, L, R),
        out_shape=jax.ShapeDtypeStruct((R, D), bf),
        in_specs=[vmem, hbm, hbm, hbm, hbm, smem, vmem],
        out_specs=vmem,
        scratch_shapes=[
            pltpu.VMEM((T, R, D), bf),
            pltpu.VMEM((3, D, width), bf),
            pltpu.VMEM((T * L, VALUE, D), bf),
            pltpu.VMEM((L, X, 2, R, 768), bf),
            pltpu.VMEM((Z, X, R, 768), bf),
            pltpu.VMEM((S * T * R, 512), bf),
            pltpu.VMEM((Z, X, R, VALUE), bf),
            pltpu.VMEM((T * L, R, VALUE), bf),
            pltpu.VMEM((L, 8, 128), f32),
            pltpu.VMEM((L, 8, 128), f32),
            pltpu.VMEM((Z, 2, X * R, VALUE), f32),
            pltpu.VMEM((Z, 2, X * R, 128), f32),
            pltpu.VMEM((Z, 2, X * R, 128), f32),
            pltpu.VMEM((R, D), f32),
            dma((3,)), dma((2,)),
            dma((3,)), dma((T,)),
            dma((1,)), dma((1,)),
            dma((2 * L - 1 + Z // 2,)), dma((2 * L - 1 + Z // 2,)),
            dma((2 * L + 1,)), dma((2 * L + 1,)),
            dma((L, X, 2)), dma((Z, X)),
            dma((3, Z, X)), dma((4, Z, X)),
            dma((Z, X)), dma((T * L,)),
        ],
        compiler_params=pltpu.CompilerParams(
            has_side_effects=True, collective_id=0, vmem_limit_bytes=60 * 1024 * 1024
        ),
    )(
        activations, query_weight, key_weight, value_weight,
        out_weight.reshape(L, VALUE, D), lambdas, head_gain.reshape(1, VALUE),
    )


def empty_state(count, local_heads):
    return (
        jnp.full((local_heads, 2, count), very_low, jnp.float32),
        jnp.zeros((local_heads, 2, count), jnp.float32),
        jnp.zeros((local_heads, 2, count, VALUE), jnp.float32),
    )


def absorb(state, query_set, query_pos, key_block, value_block, key_first):
    running, denoms, accums = state
    local_heads = running.shape[0]
    span = key_block.shape[0]
    key_grid = key_block.reshape(span, local_heads, 2, HEAD)
    scores = jnp.einsum(
        "qhme,khme->hmqk", query_set, key_grid, preferred_element_type=jnp.float32
    ) * HEAD ** (-0.5)
    key_pos = key_first + jnp.arange(span, dtype=jnp.int32)
    allowed = key_pos[None, :] <= query_pos[:, None]
    masked = jnp.where(allowed, scores, very_low)
    updated = jnp.maximum(running, jnp.max(masked, axis=-1))
    exp_weights = jnp.where(allowed, jnp.exp(masked - updated[..., None]), 0.0)
    factor = jnp.exp(running - updated)
    denoms = denoms * factor + jnp.sum(exp_weights, axis=-1)
    value_grid = value_block.reshape(span, local_heads, VALUE)
    product = jnp.einsum(
        "hmqk,khv->hmqv",
        exp_weights.astype(jnp.bfloat16),
        value_grid,
        preferred_element_type=jnp.float32,
    )
    accums = accums * factor[..., None] + product
    return (updated, denoms, accums)


def make_folder(query_sets, carry, pieces):
    key_piece, value_piece = pieces
    length = key_piece.shape[0]
    span = math.gcd(length, 512)

    def one_span(span_index, states):
        offset = span_index * span
        key_block = lax.dynamic_slice_in_dim(key_piece, offset, span, 0)
        value_block = lax.dynamic_slice_in_dim(value_piece, offset, span, 0)
        fresh = []
        for state, query_entry in zip(states, query_sets):
            query_set, query_pos = query_entry

            def take(current):
                return absorb(current, query_set, query_pos, key_block, value_block, offset)

            def leave(current):
                return current

            fresh.append(lax.cond(offset <= query_pos[-1], take, leave, state))
        return tuple(fresh)

    return lax.fori_loop(0, length // span, one_span, carry)


def shards(activations, query_weight, key_weight, value_weight, out_weight, lambdas, head_gain):
    local_heads = lambdas.shape[0]
    query_width = query_weight.shape[1]
    joined_weight = jnp.concatenate([query_weight, key_weight, value_weight], axis=1)
    projected = jnp.dot(
        lax.all_gather(activations, "tp", axis=0, tiled=True),
        joined_weight,
        preferred_element_type=jnp.float32,
    ).astype(jnp.bfloat16)
    row_count = projected.shape[0]
    queries = projected[:, :query_width].reshape(row_count, local_heads, 2, HEAD)
    key_rows = projected[:, query_width : 2 * query_width]
    value_rows = projected[:, 2 * query_width :]
    position = lax.axis_index("sp") * row_count + jnp.arange(row_count, dtype=jnp.int32)
    query_sets = [(queries, position)]
    start_states = tuple((empty_state(entry[0].shape[0], local_heads) for entry in query_sets))
    finals = make_folder(
        query_sets,
        start_states,
        (
            lax.all_gather(key_rows, "sp", axis=0, tiled=True),
            lax.all_gather(value_rows, "sp", axis=0, tiled=True),
        ),
    )
    outputs = []
    for state in finals:
        running, denoms, accums = state
        combined = (
            accums[:, 0] / denoms[:, 0, :, None]
            - lambdas[:, None, None] * accums[:, 1] / denoms[:, 1, :, None]
        )
        inverse_rms = lax.rsqrt(jnp.mean(combined * combined, axis=-1, keepdims=True) + norm_floor)
        normed = (combined * inverse_rms * head_gain).astype(jnp.bfloat16)
        outputs.append(
            jnp.transpose(normed, (1, 0, 2)).reshape(normed.shape[1], local_heads * VALUE)
        )
    heads_out = outputs[0]
    return lax.psum_scatter(
        jnp.dot(heads_out, out_weight, preferred_element_type=jnp.float32).astype(jnp.bfloat16),
        "tp",
        scatter_dimension=0,
        tiled=True,
    )


def solution(mesh):
    in_specs = (
        P(("sp", "tp"), None),
        P(None, "tp"),
        P(None, "tp"),
        P(None, "tp"),
        P("tp", None),
        P("tp"),
        P(),
    )
    out_specs = P(("sp", "tp"), None)
    S, T = mesh.shape["sp"], mesh.shape["tp"]

    def layer(*args):
        L = args[5].shape[0] // T
        rows = args[0].shape[0] // (S * T)
        fits = T == 4 and L == 2 and S == L * T and rows % 16 == 0
        local = functools.partial(fused, S, T, L) if fits else shards
        return jax.shard_map(
            local, mesh=mesh, in_specs=in_specs, out_specs=out_specs, check_vma=False
        )(*args)

    return layer
```
